128 devices in a mesh: tp: 16 (over z, y), dp: 8 (over x, core).
Axes of the slice: x: 4, y: 4, z: 4, core: 2. Of those that a mesh axis runs over, the one named last changes fastest.
Arguments:
- tokens: bfloat16 [256, 4096], P('dp', 'tp'), may hold values from -6 to 6
- lengths: int32 [256], P('dp'), may hold values from 1 to 96, 6144 in all
- norm_gain: float32 [2, 4096], replicated, may hold values from 0.1 to 1.9
- w_recept: bfloat16 [2, 4096, 4096], P(None, None, ('tp', 'dp')), may hold values from -0.09375 to 0.09375
- w_key: bfloat16 [2, 4096, 4096], P(None, None, ('tp', 'dp')), may hold values from -0.09375 to 0.09375
- w_value: bfloat16 [2, 4096, 4096], P(None, None, ('tp', 'dp')), may hold values from -0.09375 to 0.09375
- w_decay: bfloat16 [2, 4096, 4096], P(None, None, ('tp', 'dp')), may hold values from -0.09375 to 0.09375
- w_rate: bfloat16 [2, 4096, 4096], P(None, None, ('tp', 'dp')), may hold values from -0.09375 to 0.09375
- w_gate: bfloat16 [2, 4096, 4096], P(None, None, ('tp', 'dp')), may hold values from -0.09375 to 0.09375
- w_out: bfloat16 [2, 4096, 4096], P(None, None, ('tp', 'dp')), may hold values from -0.09375 to 0.09375
- decay_base: float32 [2, 4096], P(None, 'tp'), may hold values from -3 to 1
- rate_base: float32 [2, 4096], P(None, 'tp'), may hold values from -3 to 3
- group_gain: float32 [2, 4096], P(None, 'tp'), may hold values from 0.1 to 1.9
- state: float32 [2, 256, 64, 64, 64], P(None, 'dp', 'tp'), may hold values from -6 to 6
Outputs:
- mixed: bfloat16 [256, 4096], P('dp', 'tp')
- new_state: float32 [2, 256, 64, 64, 64], P(None, 'dp', 'tp')
The draws below stay inside these ranges and needn't reach their ends.
Inputs may be any that keep to these rules, and one draw needn't show every extreme that they name: Each sequence's live length lies between 1 and 96, some sequences reach 96, and the lengths sum to 6144.
All inputs are finite; a program needn't handle non-finite values.
Results may differ from the reference program's by a relative error of at most 0.025.
Values may be sent and summed in bfloat16 or wider, within the bound.
A program may use at most 128 MiB of HBM per device.

```python
import math
import jax
import jax.numpy as jnp
import numpy as np
from jax import lax

D = 4096
HEAD = 64
STEP = 16
BATCH = 256


def steps_of(key, extent, cuts, least, high):
    gain, own = 1.0, jax.random.fold_in(key, 6)
    for dim, blocks in cuts:
        heights = jnp.exp(jax.random.uniform(jax.random.fold_in(own, dim), (blocks,), jnp.float32, least / len(cuts), high / len(cuts)))
        gain = gain * jnp.repeat(heights, extent[dim] // blocks).reshape([-1 if axis == dim else 1 for axis in range(len(extent))])
    return gain


def profile(amount, total, reach, slope):
    loads = [(1 << 20) // math.isqrt(grade ** slope) + 1 for grade in range(2, amount + 1)]
    surplus, given = total - reach - (amount - 1), [1] * (amount - 1)
    while surplus > 0:
        candidates = [i for i in range(amount - 1) if given[i] < reach]
        pool, left = sum([loads[i] for i in candidates]), surplus
        for i in candidates:
            addition = min(reach - given[i], max(1, left * loads[i] // pool), surplus)
            given[i] = given[i] + addition
            surplus = surplus - addition
    return np.array([reach] + given)


def uneven_parts(key, amount, total, limit, slope):
    if amount == 2:
        one = jax.random.randint(key, (), max(1, total - limit), min(limit, total - 1) + 1)
        return jnp.stack([one, total - one])
    sizes = jnp.asarray(profile(amount, total, limit, slope), jnp.int32)
    couples = (amount - 1) // 2
    donor, receiver = sizes[1:1 + 2 * couples:2], sizes[2:2 + 2 * couples:2]
    room = jnp.minimum(donor - 1, limit - receiver)
    moved = jax.random.randint(jax.random.fold_in(key, 1), (couples,), 0, 1 << 20) % (room + 1)
    sizes = sizes.at[1:1 + 2 * couples:2].set(donor - moved).at[2:2 + 2 * couples:2].set(receiver + moved)
    return sizes[jax.random.permutation(jax.random.fold_in(key, 2), amount)]


def scatter_about(rng, dims, width, reach, pieces=(), dtype=jnp.bfloat16):
    level = steps_of(rng, dims, pieces, -0.22, 0.18) if pieces else 1.0
    values = jax.random.normal(rng, dims, jnp.float32) * width * level
    return jnp.minimum(jnp.maximum(values, -reach), reach).astype(dtype)


def setup_inputs(seed: int = 0) -> dict:
    splits = jax.random.split(jax.random.key(seed), 15)
    tokens = scatter_about(splits[0], (BATCH, D), 1.0, 6.0, ((0, 8), (1, 16)))
    lengths = uneven_parts(splits[1], BATCH, 24 * BATCH, 96, 2).astype(jnp.int32)
    norm_gain = jnp.clip(1.0 + 0.18 * jax.random.normal(splits[2], (2, D), jnp.float32), 0.1, 1.9)
    w_recept = scatter_about(splits[3], (2, D, D), D ** -0.5, 0.09375, ((2, 128),))
    w_key = scatter_about(splits[4], (2, D, D), D ** -0.5, 0.09375, ((2, 128),))
    w_value = scatter_about(splits[5], (2, D, D), D ** -0.5, 0.09375, ((2, 128),))
    w_decay = scatter_about(splits[6], (2, D, D), D ** -0.5, 0.09375, ((2, 128),))
    w_rate = scatter_about(splits[7], (2, D, D), D ** -0.5, 0.09375, ((2, 128),))
    w_gate = scatter_about(splits[8], (2, D, D), D ** -0.5, 0.09375, ((2, 128),))
    w_out = scatter_about(splits[9], (2, D, D), D ** -0.5, 0.09375, ((2, 128),))
    decay_base = jnp.clip(-3.0 + 4.0 * jax.random.uniform(splits[10], (2, D), jnp.float32) ** steps_of(splits[10], (2, D), ((1, 16),), -0.2, 0.2), -3.0, 1.0)
    rate_base = scatter_about(splits[11], (2, D), 0.5, 3.0, ((1, 16),), jnp.float32)
    group_gain = jnp.clip(1.0 + 0.18 * jax.random.normal(splits[12], (2, D), jnp.float32), 0.1, 1.9)
    state = scatter_about(splits[13], (2, BATCH, D // HEAD, HEAD, HEAD), 1.0, 6.0, ((1, 8), (2, 16)), jnp.float32)
    return dict(tokens=tokens, lengths=lengths, norm_gain=norm_gain, w_recept=w_recept, w_key=w_key, w_value=w_value, w_decay=w_decay, w_rate=w_rate, w_gate=w_gate, w_out=w_out, decay_base=decay_base, rate_base=rate_base, group_gain=group_gain, state=state)


RMS_EPS = 1e-06
GROUP_EPS = 0.00064

def stored(matrix, weight):
    product = jnp.dot(matrix, weight, preferred_element_type=jnp.float32)
    return lax.optimization_barrier(product.astype(jnp.bfloat16)).astype(jnp.float32)

def recur(state_old, recept, key_vec, value_vec, decay_rate, learn_rate, active, head_size):
    split = (recept.shape[0], -1, head_size)
    recept_h = recept.reshape(split)
    key_h = key_vec.reshape(split)
    value_h = value_vec.reshape(split)
    decay_h = decay_rate.reshape(split)
    rate_h = learn_rate.reshape(split)
    key_len = jnp.sqrt(lax.optimization_barrier(jnp.sum(key_h * key_h, axis=-1, keepdims=True)))
    key_unit = key_h / jnp.maximum(key_len, 1e-12)
    state_a = jnp.einsum('bhij,bhj->bhi', state_old, -key_unit, precision=lax.Precision.HIGHEST)
    updated = state_old * decay_h[:, :, None, :] + state_a[:, :, :, None] * (key_unit * rate_h)[:, :, None, :] + value_h[:, :, :, None] * (key_h * rate_h)[:, :, None, :]
    updated = jnp.where(active[:, None, None, None], updated, state_old)
    readout = jnp.einsum('bhij,bhj->bhi', updated, recept_h, precision=lax.Precision.HIGHEST)
    centre = lax.optimization_barrier(jnp.mean(readout, axis=-1, keepdims=True))
    spread = lax.optimization_barrier(jnp.mean(jnp.square(readout - centre), axis=-1, keepdims=True))
    normal_out = ((readout - centre) * lax.rsqrt(spread + GROUP_EPS)).reshape(recept.shape[0], -1)
    return (updated, normal_out)

def reference(tokens, lengths, norm_gain, w_recept, w_key, w_value, w_decay, w_rate, w_gate, w_out, decay_base, rate_base, group_gain, state):
    active = lengths > STEP
    current = tokens
    updated_states = []
    for layer_idx in range(2):
        values = current.astype(jnp.float32)
        factor = lax.rsqrt(lax.optimization_barrier(jnp.mean(values * values, axis=1, keepdims=True)) + RMS_EPS)
        normed = (values * factor * norm_gain[layer_idx]).astype(jnp.bfloat16)
        recept = stored(normed, w_recept[layer_idx])
        key_vec = stored(normed, w_key[layer_idx])
        value_vec = stored(normed, w_value[layer_idx])
        decay_pre = stored(normed, w_decay[layer_idx])
        rate_pre = stored(normed, w_rate[layer_idx])
        gate_pre = stored(normed, w_gate[layer_idx])
        decay_rate = jnp.exp(-jnp.exp(-jax.nn.softplus(-(decay_base[layer_idx] + decay_pre)) - 0.5))
        learn_rate = jax.nn.sigmoid(rate_base[layer_idx] + rate_pre)
        gate_open = jax.nn.sigmoid(gate_pre)
        updated, normal_out = recur(state[layer_idx], recept, key_vec, value_vec, decay_rate, learn_rate, active, HEAD)
        updated_states.append(updated)
        mixed_rows = jnp.where(active[:, None], normal_out * group_gain[layer_idx] * gate_open, 0.0).astype(jnp.bfloat16)
        current = jnp.dot(mixed_rows, w_out[layer_idx], preferred_element_type=jnp.float32).astype(jnp.bfloat16)
    return (current, jnp.stack(updated_states))
```

```python
import math

import jax
import jax.numpy as jnp
from jax import lax
from jax.experimental import pallas as pl
from jax.experimental.pallas import tpu as pltpu
from jax.sharding import Mesh
from jax.sharding import PartitionSpec as P

STEP = 16
RMS_EPS = 1e-06
GROUP_EPS = 0.00064
MESH = pl.DeviceIdType.MESH
AXES = ("z", "y", "x")
ORDERS = ((2, 1, 0), (1, 0, 2), (0, 2, 1), (1, 2, 0))
NT = (((1,), (1,)), ((), ()))
F32 = jnp.float32
BF16 = jnp.bfloat16
DECAY_SCALE = math.exp(-0.5)


def kernel(
    tokens,
    lengths,
    norm_gain,
    w_recept,
    w_key,
    w_value,
    w_decay,
    w_rate,
    w_gate,
    w_out,
    decay_base,
    rate_base,
    group_gain,
    state,
    mixed_out,
    state_out,
    g0,
    g1,
    g2,
    g3,
    wp,
    wo,
    st,
    a2a_s,
    a2a_r,
    fin_s,
    fin_r,
    u_ref,
    w_ref,
    kl_ref,
    tok_sem,
    loc_sem,
    sib_send,
    sib_recv,
    st_sem,
    g_send,
    g_recv,
    x_send,
    x_recv,
):
    me = tuple(lax.axis_index(axis) for axis in AXES)
    core = lax.axis_index("core")
    weights = (w_recept, w_key, w_value, w_decay, w_rate, w_gate, w_out)

    def peer(dim, step):
        return lax.rem(me[dim] + step, 4)

    def device(dim, step):
        return {AXES[dim]: peer(dim, step)}

    sibling = {"core": 1 - core}

    def remote(src, dst, send, recv, where):
        return pltpu.make_async_remote_copy(
            src_ref=src, dst_ref=dst, send_sem=send, recv_sem=recv, device_id=where, device_id_type=MESH
        )

    own = pltpu.make_async_copy(tokens, g0.at[me[0], me[1], me[2]], tok_sem)
    own.start()

    def weight_dst(layer, mat):
        if mat == 6:
            return wo.at[layer, core]
        return wp.at[layer, 2 * mat + core]

    def weight_src(layer, mat):
        return weights[mat].at[layer]

    def local_weight(layer, mat):
        return pltpu.make_async_copy(
            weight_src(layer, mat), weight_dst(layer, mat), loc_sem.at[layer, mat]
        )

    def sibling_weight(layer, mat):
        return remote(
            weight_src(layer, mat),
            weight_dst(layer, mat),
            sib_send.at[layer, mat],
            sib_recv.at[layer, mat],
            sibling,
        )

    def state_in(layer):
        return pltpu.make_async_copy(state.at[layer], st.at[layer], st_sem.at[0, layer])

    def state_back(layer):
        return pltpu.make_async_copy(st.at[layer], state_out.at[layer], st_sem.at[1, layer])

    barrier = pltpu.get_barrier_semaphore()
    for dim in range(3):
        for step in range(1, 4):
            pl.semaphore_signal(barrier, inc=1, device_id=device(dim, step), device_id_type=MESH)
    pl.semaphore_signal(barrier, inc=1, device_id=sibling, device_id_type=MESH)
    for mat in range(6):
        local_weight(0, mat).start()
    pl.semaphore_wait(barrier, 10)

    def region(buf, sub, sel):
        where = tuple(pl.ds(start, size) for start, size in sel)
        if buf.shape[-1] == 256:
            tile = (pl.ds(16 * (sub // 2), 16), pl.ds(128 * (sub % 2), 128))
        else:
            tile = (pl.ds(16 * sub, 16), pl.ds(0, 128))
        return buf.at[where + tile]

    def selection(parts):
        return tuple(parts[dim] for dim in range(3))

    def send(gid, buf, sub, stage, slot, sel, dim, step):
        block = region(buf, sub, sel)
        remote(block, block, g_send.at[gid, sub, stage], g_recv.at[gid, sub, slot], device(dim, step)).start()

    def arrived(gid, buf, sub, slot, sel):
        block = region(buf, sub, sel)
        remote(block, block, g_send.at[gid, sub, 0], g_recv.at[gid, sub, slot], sibling).wait_recv()

    def own_sel(dim_sel):
        return selection([dim_sel.get(dim, (me[dim], 1)) for dim in range(3)])

    def stage_one(gid, buf):
        for step in (1, 3, 2):
            for sub, (one, two, three) in enumerate(ORDERS):
                send(gid, buf, sub, 0, step - 1, own_sel({}), one, step)

    def stage_two(gid, buf):
        for sub, (one, two, three) in enumerate(ORDERS):
            for step in range(1, 4):
                arrived(gid, buf, sub, step - 1, own_sel({one: (peer(one, 4 - step), 1)}))
            for step in (1, 3, 2):
                send(gid, buf, sub, 1, 2 + step, own_sel({one: (0, 4)}), two, step)

    def stage_three(gid, buf):
        for sub, (one, two, three) in enumerate(ORDERS):
            for step in range(1, 4):
                arrived(gid, buf, sub, 2 + step, own_sel({one: (0, 4), two: (peer(two, 4 - step), 1)}))
            low = own_sel({one: (0, 2), two: (0, 4)})
            high = own_sel({one: (2, 2), two: (0, 4)})
            send(gid, buf, sub, 2, 6, low, three, 1)
            send(gid, buf, sub, 2, 8, high, three, 3)
            send(gid, buf, sub, 2, 7, high, three, 1)
            send(gid, buf, sub, 2, 9, low, three, 3)

    def stage_four(gid, buf):
        for sub, (one, two, three) in enumerate(ORDERS):
            low = own_sel({one: (0, 2), two: (0, 4), three: (peer(three, 3), 1)})
            arrived(gid, buf, sub, 6, low)
            send(gid, buf, sub, 2, 10, low, three, 1)
            high = own_sel({one: (2, 2), two: (0, 4), three: (peer(three, 1), 1)})
            arrived(gid, buf, sub, 8, high)
            send(gid, buf, sub, 2, 11, high, three, 3)

    def stage_five(gid, buf):
        for sub, (one, two, three) in enumerate(ORDERS):
            arrived(gid, buf, sub, 7, own_sel({one: (2, 2), two: (0, 4), three: (peer(three, 3), 1)}))
            arrived(gid, buf, sub, 9, own_sel({one: (0, 2), two: (0, 4), three: (peer(three, 1), 1)}))
            arrived(gid, buf, sub, 10, own_sel({one: (0, 2), two: (0, 4), three: (peer(three, 2), 1)}))
            arrived(gid, buf, sub, 11, own_sel({one: (2, 2), two: (0, 4), three: (peer(three, 2), 1)}))

    def gather_drain(gid, buf):
        for sub, (one, two, three) in enumerate(ORDERS):
            for stage, sel in enumerate(
                ({one: (0, 3)}, {one: (0, 4), two: (0, 3)}, {one: (0, 4), two: (0, 4), three: (0, 3)})
            ):
                parts = selection([sel.get(dim, (0, 1)) for dim in range(3)])
                block = region(buf, sub, parts)
                remote(block, block, g_send.at[gid, sub, stage], g_recv.at[gid, sub, 0], sibling).wait_send()

    def exchange(eid, src, dst):
        for step in (1, 3, 2):
            remote(
                src.at[peer(2, step)],
                dst.at[me[2]],
                x_send.at[eid, step - 1],
                x_recv.at[eid, step - 1],
                device(2, step),
            ).start()

    def exchange_wait(eid, src, dst):
        for step in range(1, 4):
            slot = dst.at[peer(2, 4 - step)]
            remote(slot, slot, x_send.at[eid, step - 1], x_recv.at[eid, step - 1], sibling).wait_recv()

    def exchange_drain(eid, src, dst):
        for step in range(1, 4):
            slot = src.at[peer(2, step)]
            remote(slot, slot, x_send.at[eid, step - 1], x_recv.at[eid, step - 1], sibling).wait_send()

    def weights_ready(layer, mats):
        for mat in mats:
            local_weight(layer, mat).wait()
            remote(
                weight_src(layer, mat),
                other_dst(layer, mat),
                sib_send.at[layer, mat],
                sib_recv.at[layer, mat],
                sibling,
            ).wait_recv()

    def other_dst(layer, mat):
        if mat == 6:
            return wo.at[layer, 1 - core]
        return wp.at[layer, 2 * mat + 1 - core]

    def scale_weights(layer):
        def body(idx, carry):
            for part in range(4):
                cols = slice(1024 * part, 1024 * (part + 1))
                gain = norm_gain[layer : layer + 1, cols]
                wp[layer, idx, :, cols] = (wp[layer, idx, :, cols].astype(F32) * gain).astype(BF16)
            return carry

        lax.fori_loop(0, 12, body, 0)

    ones = jnp.ones((8, 256), BF16)

    def project(layer, buf):
        acc = jnp.zeros((384, 128), F32)
        squares = jnp.zeros((8, 128), F32)
        for group in range(16):
            weight = wp[layer, :, :, 256 * group : 256 * (group + 1)].reshape(384, 256)
            if layer == 0:
                block = buf[group // 4, group % 4].reshape(128, 256)
                acc += lax.dot_general(weight, block, NT, preferred_element_type=F32)
                squares += lax.dot_general(ones, block * block, NT, preferred_element_type=F32)
            else:
                block = buf[group // 4, group % 4].reshape(256, 128)
                acc += jnp.dot(weight, block, preferred_element_type=F32)
                squares += jnp.dot(ones, block * block, preferred_element_type=F32)
        factor = lax.rsqrt(squares[0:1, :] * (1.0 / 4096) + RMS_EPS)
        rows = jnp.transpose(acc * factor).astype(BF16)
        a2a_s[layer] = rows.reshape(4, 32, 384)

    def head_parts(row):
        return [row[:, 64 * head : 64 * (head + 1)] for head in range(4)]

    lane_len = lengths[...].astype(F32)
    diag = lax.broadcasted_iota(jnp.int32, (32, 32), 0) == lax.broadcasted_iota(jnp.int32, (32, 32), 1)
    active = jnp.sum(jnp.where(diag, lane_len, 0.0), axis=1, keepdims=True) > STEP
    row_of = lax.broadcasted_iota(jnp.int32, (8, 64), 0)

    def recur(layer):
        decay_parts = head_parts(decay_base[layer : layer + 1, :])
        rate_parts = head_parts(rate_base[layer : layer + 1, :])
        gain_parts = head_parts(group_gain[layer : layer + 1, :])
        results = []
        for head in range(4):
            tile = a2a_r[layer, head].astype(F32)
            recept, key, value, decay, rate, gate = [
                tile[:, 64 * mat : 64 * (mat + 1)] for mat in range(6)
            ]
            size = jnp.maximum(jnp.sqrt(jnp.sum(key * key, axis=1, keepdims=True)), 1e-12)
            unit = key / size
            keep = jnp.exp(-DECAY_SCALE * jax.nn.sigmoid(decay_parts[head] + decay))
            unit_rate = unit * jax.nn.sigmoid(rate_parts[head] + rate)
            beta = jnp.sum(unit_rate * recept, axis=1, keepdims=True)
            probe = (keep * recept).astype(BF16)
            unit_b = unit.astype(BF16)
            along, read = [], []
            for octet in range(4):
                rows = slice(8 * octet, 8 * octet + 8)
                left = jnp.concatenate([unit_b[rows], probe[rows]], axis=0)
                sum_a = jnp.zeros((8, 64), F32)
                sum_r = jnp.zeros((8, 64), F32)
                for low in range(8):
                    seq = 8 * octet + low
                    matrix = st[layer, seq, head].astype(BF16)
                    both = lax.dot_general(left, matrix, NT, preferred_element_type=F32)
                    sum_a = jnp.where(row_of == low, both[0:8], sum_a)
                    sum_r = jnp.where(row_of == low, both[8:16], sum_r)
                along.append(sum_a)
                read.append(sum_r)
            delta = size * value - jnp.concatenate(along, axis=0)
            readout = jnp.concatenate(read, axis=0) + delta * beta
            centre = jnp.mean(readout, axis=1, keepdims=True)
            moved = readout - centre
            spread = jnp.mean(moved * moved, axis=1, keepdims=True)
            normal = moved * lax.rsqrt(spread + GROUP_EPS) * gain_parts[head]
            results.append(jnp.where(active, normal * jax.nn.sigmoid(gate), 0.0))
            u_ref[head] = jnp.transpose(delta)
            w_ref[head] = jnp.where(active, keep, 1.0)
            kl_ref[head] = jnp.where(active, unit_rate, 0.0)
        return jnp.concatenate(results, axis=1).astype(BF16)

    def update_state(layer):
        for head in range(4):
            column = u_ref[head]
            for seq in range(32):
                st[layer, seq, head] = (
                    st[layer, seq, head] * w_ref[head, seq : seq + 1, :]
                    + column[:, seq : seq + 1] * kl_ref[head, seq : seq + 1, :]
                )

    def output(layer, buf):
        acc = jnp.zeros((64, 128), F32)
        for group in range(16):
            weight = wo[layer, :, :, 256 * group : 256 * (group + 1)].reshape(64, 256)
            block = buf[group // 4, group % 4].reshape(128, 256)
            acc += lax.dot_general(weight, block, NT, preferred_element_type=F32)
        return acc

    def store_own(buf, value):
        buf[me[0], me[1], me[2]] = value

    own.wait()
    stage_one(0, g0)
    for mat in range(6):
        sibling_weight(0, mat).start()
    state_in(0).start()
    local_weight(0, 6).start()
    sibling_weight(0, 6).start()
    stage_two(0, g0)
    stage_three(0, g0)
    for mat in range(7):
        local_weight(1, mat).start()
        sibling_weight(1, mat).start()
    state_in(1).start()
    weights_ready(0, range(6))
    stage_four(0, g0)
    scale_weights(0)
    stage_five(0, g0)
    project(0, g0)
    exchange(0, a2a_s.at[0], a2a_r.at[0])
    a2a_r[0, me[2]] = a2a_s[0, me[2]]
    state_in(0).wait()
    exchange_wait(0, a2a_s.at[0], a2a_r.at[0])
    store_own(g1, recur(0))
    stage_one(1, g1)
    weights_ready(0, (6,))
    stage_two(1, g1)
    stage_three(1, g1)
    stage_four(1, g1)
    update_state(0)
    state_back(0).start()
    stage_five(1, g1)
    store_own(g2, output(0, g1).astype(BF16))
    stage_one(2, g2)
    weights_ready(1, range(7))
    stage_two(2, g2)
    stage_three(2, g2)
    stage_four(2, g2)
    scale_weights(1)
    stage_five(2, g2)
    project(1, g2)
    exchange(1, a2a_s.at[1], a2a_r.at[1])
    a2a_r[1, me[2]] = a2a_s[1, me[2]]
    state_in(1).wait()
    exchange_wait(1, a2a_s.at[1], a2a_r.at[1])
    store_own(g3, recur(1))
    stage_one(3, g3)
    stage_two(3, g3)
    stage_three(3, g3)
    stage_four(3, g3)
    update_state(1)
    state_back(1).start()
    stage_five(3, g3)
    fin_s[...] = jnp.transpose(output(1, g3)).astype(BF16).reshape(4, 32, 64)
    exchange(2, fin_s, fin_r)
    fin_r[me[2]] = fin_s[me[2]]
    exchange_wait(2, fin_s, fin_r)
    mixed_out[...] = jnp.concatenate([fin_r[head].astype(F32) for head in range(4)], axis=1).astype(BF16)
    for layer in range(2):
        for mat in range(7):
            sibling_weight(layer, mat).wait_send()
    for gid, buf in enumerate((g0, g1, g2, g3)):
        gather_drain(gid, buf)
    exchange_drain(0, a2a_s.at[0], a2a_r.at[0])
    exchange_drain(1, a2a_s.at[1], a2a_r.at[1])
    exchange_drain(2, fin_s, fin_r)
    state_back(0).wait()
    state_back(1).wait()


def local(tokens, lengths, norm_gain, *rest):
    weights = [jnp.swapaxes(weight, 1, 2) for weight in rest[:7]]
    decay_base, rate_base, group_gain, state = rest[7:]
    vmem = pl.BlockSpec(memory_space=pltpu.VMEM)
    anywhere = pl.BlockSpec(memory_space=pl.ANY)
    rows_block = pltpu.VMEM((4, 4, 4, 32, 256), BF16)
    dma = pltpu.SemaphoreType.DMA
    return pl.pallas_call(
        kernel,
        out_shape=(
            jax.ShapeDtypeStruct((32, 256), BF16),
            jax.ShapeDtypeStruct(state.shape, F32),
        ),
        in_specs=[anywhere, vmem, vmem] + [anywhere] * 7 + [vmem] * 3 + [anywhere],
        out_specs=(vmem, anywhere),
        scratch_shapes=[
            rows_block,
            rows_block,
            pltpu.VMEM((4, 4, 4, 64, 128), BF16),
            rows_block,
            pltpu.VMEM((2, 12, 32, 4096), BF16),
            pltpu.VMEM((2, 2, 32, 4096), BF16),
            pltpu.VMEM((2, 32, 4, 64, 64), F32),
            pltpu.VMEM((2, 4, 32, 384), BF16),
            pltpu.VMEM((2, 4, 32, 384), BF16),
            pltpu.VMEM((4, 32, 64), BF16),
            pltpu.VMEM((4, 32, 64), BF16),
            pltpu.VMEM((4, 64, 32), F32),
            pltpu.VMEM((4, 32, 64), F32),
            pltpu.VMEM((4, 32, 64), F32),
            dma,
            dma((2, 7)),
            dma((2, 7)),
            dma((2, 7)),
            dma((2, 2)),
            dma((4, 4, 3)),
            dma((4, 4, 12)),
            dma((3, 3)),
            dma((3, 3)),
        ],
        compiler_params=pltpu.CompilerParams(
            collective_id=0, has_side_effects=True, vmem_limit_bytes=60 * 1024 * 1024
        ),
    )(tokens, lengths.reshape(1, 32), norm_gain, *weights, decay_base, rate_base, group_gain, state)


def solution(mesh):
    finer = Mesh(mesh.devices.reshape(4, 4, 4, 2), ("z", "y", "x", "core"))
    tp, dp = ("z", "y"), ("x", "core")
    weight = P(None, None, tp + dp)
    vector = P(None, tp)
    states = P(None, dp, tp, None, None)
    in_specs = (P(dp, tp), P(dp), P()) + (weight,) * 7 + (vector,) * 3 + (states,)
    return jax.shard_map(
        local, mesh=finer, in_specs=in_specs, out_specs=(P(dp, tp), states), check_vma=False
    )
```

```python
import math

import jax
import jax.numpy as jnp
from jax import lax
from jax.experimental import pallas as pl
from jax.experimental.pallas import tpu as pltpu
from jax.sharding import Mesh
from jax.sharding import PartitionSpec as P

STEP = 16
RMS_EPS = 1e-06
GROUP_EPS = 0.00064
MESH = pl.DeviceIdType.MESH
AXES = ("z", "y", "x")
ORDERS = ((2, 1, 0), (1, 0, 2), (0, 2, 1), (1, 2, 0))
PLANE = sorted(
    [(dz, dy) for dz in range(4) for dy in range(4) if dz or dy],
    key=lambda offset: -min(offset[0], 4 - offset[0]) - min(offset[1], 4 - offset[1]),
)
NT = (((1,), (1,)), ((), ()))
F32 = jnp.float32
BF16 = jnp.bfloat16
DECAY_SCALE = math.exp(-0.5)


def kernel(
    tokens,
    lengths_hbm,
    norm_gain_hbm,
    w_recept,
    w_key,
    w_value,
    w_decay,
    w_rate,
    w_gate,
    w_out,
    decay_base_hbm,
    rate_base_hbm,
    group_gain_hbm,
    state,
    mixed_out,
    st,
    g0,
    g1,
    g2,
    g3,
    wp,
    wo,
    a2a_s,
    a2a_r,
    u_ref,
    w_ref,
    kl_ref,
    lengths,
    norm_gain,
    decay_base,
    rate_base,
    group_gain,
    tok_sem,
    small_sem,
    loc_sem,
    sib_send,
    sib_recv,
    st_sem,
    g_send,
    g_recv,
    p_send,
    p_recv,
    r_send,
    r_recv,
    d_send,
    d_recv,
    x_send,
    x_recv,
):
    me = tuple(lax.axis_index(axis) for axis in AXES)
    core = lax.axis_index("core")
    weights = (w_recept, w_key, w_value, w_decay, w_rate, w_gate, w_out)

    def peer(dim, step):
        return lax.rem(me[dim] + step, 4)

    def device(dim, step):
        return {AXES[dim]: peer(dim, step)}

    def plane_device(dz, dy):
        return {"z": peer(0, dz), "y": peer(1, dy)}

    sibling = {"core": 1 - core}

    def remote(src, dst, send, recv, where):
        return pltpu.make_async_remote_copy(
            src_ref=src, dst_ref=dst, send_sem=send, recv_sem=recv, device_id=where, device_id_type=MESH
        )

    own = pltpu.make_async_copy(tokens, g0.at[me[0], me[1], me[2]], tok_sem)
    own.start()

    def weight_dst(layer, mat):
        if mat == 6:
            return wo.at[layer, me[2], core]
        return wp.at[layer, 2 * mat + core]

    def weight_src(layer, mat):
        return weights[mat].at[layer]

    def local_weight(layer, mat):
        return pltpu.make_async_copy(
            weight_src(layer, mat), weight_dst(layer, mat), loc_sem.at[layer, mat]
        )

    def sibling_weight(layer, mat):
        return remote(
            weight_src(layer, mat),
            weight_dst(layer, mat),
            sib_send.at[layer, mat],
            sib_recv.at[layer, mat],
            sibling,
        )

    def state_in(layer):
        return pltpu.make_async_copy(state.at[layer], st.at[layer], st_sem.at[layer])

    barrier = pltpu.get_barrier_semaphore()
    partners = [device(2, step) for step in range(1, 4)] + [plane_device(*offset) for offset in PLANE] + [sibling]
    for partner in partners:
        pl.semaphore_signal(barrier, inc=1, device_id=partner, device_id_type=MESH)
    for mat in range(6):
        local_weight(0, mat).start()
    small = [
        pltpu.make_async_copy(src, dst, small_sem.at[idx])
        for idx, (src, dst) in enumerate(
            (
                (norm_gain_hbm, norm_gain),
                (lengths_hbm, lengths),
                (decay_base_hbm, decay_base),
                (rate_base_hbm, rate_base),
                (group_gain_hbm, group_gain),
            )
        )
    ]
    for copy in small:
        copy.start()
    pl.semaphore_wait(barrier, len(partners))

    def region(buf, sub, sel):
        where = tuple(pl.ds(start, size) for start, size in sel)
        tile = (pl.ds(16 * (sub // 2), 16), pl.ds(128 * (sub % 2), 128))
        return buf.at[where + tile]

    def selection(parts):
        return tuple(parts[dim] for dim in range(3))

    def send(gid, buf, sub, stage, slot, sel, dim, step):
        block = region(buf, sub, sel)
        remote(block, block, g_send.at[gid, sub, stage], g_recv.at[gid, sub, slot], device(dim, step)).start()

    def arrived(gid, buf, sub, slot, sel):
        block = region(buf, sub, sel)
        remote(block, block, g_send.at[gid, sub, 0], g_recv.at[gid, sub, slot], sibling).wait_recv()

    def own_sel(dim_sel):
        return selection([dim_sel.get(dim, (me[dim], 1)) for dim in range(3)])

    def stage_one(gid, buf):
        for step in (1, 3, 2):
            for sub, (one, two, three) in enumerate(ORDERS):
                send(gid, buf, sub, 0, step - 1, own_sel({}), one, step)

    def stage_two(gid, buf):
        for sub, (one, two, three) in enumerate(ORDERS):
            for step in range(1, 4):
                arrived(gid, buf, sub, step - 1, own_sel({one: (peer(one, 4 - step), 1)}))
            for step in (1, 3, 2):
                send(gid, buf, sub, 1, 2 + step, own_sel({one: (0, 4)}), two, step)

    def stage_three(gid, buf):
        for sub, (one, two, three) in enumerate(ORDERS):
            for step in range(1, 4):
                arrived(gid, buf, sub, 2 + step, own_sel({one: (0, 4), two: (peer(two, 4 - step), 1)}))
            low = own_sel({one: (0, 2), two: (0, 4)})
            high = own_sel({one: (2, 2), two: (0, 4)})
            send(gid, buf, sub, 2, 6, low, three, 1)
            send(gid, buf, sub, 2, 8, high, three, 3)
            send(gid, buf, sub, 2, 7, high, three, 1)
            send(gid, buf, sub, 2, 9, low, three, 3)

    def stage_four(gid, buf):
        for sub, (one, two, three) in enumerate(ORDERS):
            low = own_sel({one: (0, 2), two: (0, 4), three: (peer(three, 3), 1)})
            arrived(gid, buf, sub, 6, low)
            send(gid, buf, sub, 2, 10, low, three, 1)
            high = own_sel({one: (2, 2), two: (0, 4), three: (peer(three, 1), 1)})
            arrived(gid, buf, sub, 8, high)
            send(gid, buf, sub, 2, 11, high, three, 3)

    def stage_five(gid, buf):
        for sub, (one, two, three) in enumerate(ORDERS):
            arrived(gid, buf, sub, 7, own_sel({one: (2, 2), two: (0, 4), three: (peer(three, 3), 1)}))
            arrived(gid, buf, sub, 9, own_sel({one: (0, 2), two: (0, 4), three: (peer(three, 1), 1)}))
            arrived(gid, buf, sub, 10, own_sel({one: (0, 2), two: (0, 4), three: (peer(three, 2), 1)}))
            arrived(gid, buf, sub, 11, own_sel({one: (2, 2), two: (0, 4), three: (peer(three, 2), 1)}))

    def gather_drain(gid, buf):
        for sub, (one, two, three) in enumerate(ORDERS):
            for stage, sel in enumerate(
                ({one: (0, 3)}, {one: (0, 4), two: (0, 3)}, {one: (0, 4), two: (0, 4), three: (0, 3)})
            ):
                parts = selection([sel.get(dim, (0, 1)) for dim in range(3)])
                block = region(buf, sub, parts)
                remote(block, block, g_send.at[gid, sub, stage], g_recv.at[gid, sub, 0], sibling).wait_send()

    def plane_start(pid, buf):
        block = buf.at[me[0], me[1]]
        for dz, dy in PLANE:
            remote(
                block, block, p_send.at[pid, min(dz, 1)], p_recv.at[pid, 4 * dz + dy - 1], plane_device(dz, dy)
            ).start()

    def plane_wait(pid, buf):
        for dz, dy in PLANE[::-1]:
            block = buf.at[peer(0, 4 - dz), peer(1, 4 - dy)]
            remote(block, block, p_send.at[pid, 0], p_recv.at[pid, 4 * dz + dy - 1], sibling).wait_recv()

    def plane_drain(pid, buf):
        for idx, block in enumerate((buf.at[pl.ds(0, 1), pl.ds(0, 3)], buf.at[pl.ds(0, 3)])):
            remote(block, block, p_send.at[pid, idx], p_recv.at[pid, 0], sibling).wait_send()

    def half(ref, part):
        return ref.at[pl.ds(16 * part, 16)]

    def ring_start(layer):
        for step, part, slot in ((1, 0, 0), (3, 1, 2), (1, 1, 1), (3, 0, 3)):
            remote(
                half(w_out.at[layer], part),
                half(wo.at[layer, me[2], core], part),
                r_send.at[layer, slot],
                r_recv.at[layer, slot],
                device(2, step),
            ).start()

    RING = ((3, 0), (3, 1), (1, 1), (1, 0), (2, 0), (2, 1))

    def ring_wait(layer, slot):
        step, part = RING[slot]
        piece = half(wo.at[layer, peer(2, step), core], part)
        remote(piece, piece, r_send.at[layer, slot], r_recv.at[layer, slot], sibling).wait_recv()

    def ring_pass(layer):
        for slot, onward, step in ((0, 4, 1), (2, 5, 3)):
            ring_wait(layer, slot)
            source, part = RING[slot]
            piece = half(wo.at[layer, peer(2, source), core], part)
            remote(piece, piece, r_send.at[layer, onward], r_recv.at[layer, onward], device(2, step)).start()

    def across(layer, step, which):
        piece = wo.at[layer, peer(2, step), which]
        return remote(piece, piece, d_send.at[layer, step - 1], d_recv.at[layer, step - 1], sibling)

    def ring_near(layer):
        ring_wait(layer, 1)
        across(layer, 3, core).start()
        ring_wait(layer, 3)
        across(layer, 1, core).start()

    def ring_far(layer):
        ring_wait(layer, 4)
        ring_wait(layer, 5)
        across(layer, 2, core).start()

    def ring_done(layer):
        for step in (3, 1, 2):
            across(layer, step, 1 - core).wait_recv()

    def ring_drain(layer):
        for step in (3, 1, 2):
            across(layer, step, core).wait_send()
        for slot in range(6):
            piece = half(wo.at[layer, 0, 0], 0)
            remote(piece, piece, r_send.at[layer, slot], r_recv.at[layer, slot], sibling).wait_send()

    def exchange(eid, src, dst):
        for step in (1, 3, 2):
            remote(
                src.at[peer(2, step)],
                dst.at[me[2]],
                x_send.at[eid, step - 1],
                x_recv.at[eid, step - 1],
                device(2, step),
            ).start()

    def exchange_wait(eid, src, dst):
        for step in range(1, 4):
            slot = dst.at[peer(2, 4 - step)]
            remote(slot, slot, x_send.at[eid, step - 1], x_recv.at[eid, step - 1], sibling).wait_recv()

    def exchange_drain(eid, src, dst):
        for step in range(1, 4):
            slot = src.at[peer(2, step)]
            remote(slot, slot, x_send.at[eid, step - 1], x_recv.at[eid, step - 1], sibling).wait_send()

    def weights_ready(layer, mats):
        for mat in mats:
            local_weight(layer, mat).wait()
            remote(
                weight_src(layer, mat),
                other_dst(layer, mat),
                sib_send.at[layer, mat],
                sib_recv.at[layer, mat],
                sibling,
            ).wait_recv()

    def other_dst(layer, mat):
        if mat == 6:
            return wo.at[layer, me[2], 1 - core]
        return wp.at[layer, 2 * mat + 1 - core]

    def scale_weights(layer):
        def body(idx, carry):
            for part in range(4):
                cols = slice(1024 * part, 1024 * (part + 1))
                gain = norm_gain[layer : layer + 1, cols]
                wp[layer, idx, :, cols] = (wp[layer, idx, :, cols].astype(F32) * gain).astype(BF16)
            return carry

        lax.fori_loop(0, 12, body, 0)

    ones = jnp.ones((8, 256), BF16)

    def project(layer, buf):
        acc = jnp.zeros((384, 128), F32)
        squares = jnp.zeros((8, 128), F32)
        for group in range(16):
            weight = wp[layer, :, :, 256 * group : 256 * (group + 1)].reshape(384, 256)
            block = buf[group // 4, group % 4].reshape(128, 256)
            acc += lax.dot_general(weight, block, NT, preferred_element_type=F32)
            squares += lax.dot_general(ones, block * block, NT, preferred_element_type=F32)
        factor = lax.rsqrt(squares[0:1, :] * (1.0 / 4096) + RMS_EPS)
        rows = jnp.transpose(acc * factor).astype(BF16)
        a2a_s[layer] = rows.reshape(4, 32, 384)

    def head_parts(row):
        return [row[:, 64 * head : 64 * (head + 1)] for head in range(4)]

    row_of = lax.broadcasted_iota(jnp.int32, (8, 64), 0)

    def recur(layer):
        lane_len = lengths[...].astype(F32)
        diag = lax.broadcasted_iota(jnp.int32, (32, 32), 0) == lax.broadcasted_iota(jnp.int32, (32, 32), 1)
        active = jnp.sum(jnp.where(diag, lane_len, 0.0), axis=1, keepdims=True) > STEP
        decay_parts = head_parts(decay_base[layer : layer + 1, :])
        rate_parts = head_parts(rate_base[layer : layer + 1, :])
        gain_parts = head_parts(group_gain[layer : layer + 1, :])
        results = []
        for head in range(4):
            tile = a2a_r[layer, head].astype(F32)
            recept, key, value, decay, rate, gate = [
                tile[:, 64 * mat : 64 * (mat + 1)] for mat in range(6)
            ]
            size = jnp.maximum(jnp.sqrt(jnp.sum(key * key, axis=1, keepdims=True)), 1e-12)
            unit = key / size
            keep = jnp.exp(-DECAY_SCALE * jax.nn.sigmoid(decay_parts[head] + decay))
            unit_rate = unit * jax.nn.sigmoid(rate_parts[head] + rate)
            beta = jnp.sum(unit_rate * recept, axis=1, keepdims=True)
            probe = (keep * recept).astype(BF16)
            unit_b = unit.astype(BF16)
            along, read = [], []
            for octet in range(4):
                rows = slice(8 * octet, 8 * octet + 8)
                left = jnp.concatenate([unit_b[rows], probe[rows]], axis=0)
                sum_a = jnp.zeros((8, 64), F32)
                sum_r = jnp.zeros((8, 64), F32)
                for low in range(8):
                    seq = 8 * octet + low
                    matrix = st[layer, seq, head].astype(BF16)
                    both = lax.dot_general(left, matrix, NT, preferred_element_type=F32)
                    sum_a = jnp.where(row_of == low, both[0:8], sum_a)
                    sum_r = jnp.where(row_of == low, both[8:16], sum_r)
                along.append(sum_a)
                read.append(sum_r)
            delta = size * value - jnp.concatenate(along, axis=0)
            readout = jnp.concatenate(read, axis=0) + delta * beta
            centre = jnp.mean(readout, axis=1, keepdims=True)
            moved = readout - centre
            spread = jnp.mean(moved * moved, axis=1, keepdims=True)
            normal = moved * lax.rsqrt(spread + GROUP_EPS) * gain_parts[head]
            results.append(jnp.where(active, normal * jax.nn.sigmoid(gate), 0.0))
            u_ref[head] = jnp.transpose(delta)
            w_ref[head] = jnp.where(active, keep, 1.0)
            kl_ref[head] = jnp.where(active, unit_rate, 0.0)
        return jnp.concatenate(results, axis=1).astype(BF16)

    def update_state(layer):
        for head in range(4):
            column = u_ref[head]
            for seq in range(32):
                st[layer, seq, head] = (
                    st[layer, seq, head] * w_ref[head, seq : seq + 1, :]
                    + column[:, seq : seq + 1] * kl_ref[head, seq : seq + 1, :]
                )

    def output(layer, buf):
        acc = jnp.zeros((256, 32), F32)
        for group in range(16):
            weight = wo[layer, :, :, :, 256 * group : 256 * (group + 1)].reshape(256, 256)
            acc += lax.dot_general(weight, buf[group // 4, group % 4], NT, preferred_element_type=F32)
        return jnp.transpose(acc).astype(BF16)

    def start_weights(layer, mats):
        for mat in mats:
            local_weight(layer, mat).start()
            sibling_weight(layer, mat).start()

    def drain_weights(layer):
        for mat in range(7):
            sibling_weight(layer, mat).wait_send()

    scope = jax.named_scope
    with scope("g0_one"):
        own.wait()
        stage_one(0, g0)
        for mat in range(6):
            sibling_weight(0, mat).start()
        state_in(0).start()
        start_weights(0, (6,))
    buffers = ((g0, g1), (g2, g3))
    for layer in range(2):
        wide, rows = buffers[layer]
        with scope("two"):
            stage_two(layer, wide)
        with scope("three"):
            stage_three(layer, wide)
            if layer == 0:
                for copy in small:
                    copy.wait()
                start_weights(1, range(7))
                state_in(1).start()
        with scope("four"):
            stage_four(layer, wide)
        with scope("scale"):
            weights_ready(layer, range(7))
            scale_weights(layer)
            drain_weights(layer)
        with scope("five"):
            stage_five(layer, wide)
        with scope("project"):
            project(layer, wide)
        with scope("exchange"):
            exchange(layer, a2a_s.at[layer], a2a_r.at[layer])
            a2a_r[layer, me[2]] = a2a_s[layer, me[2]]
            gather_drain(layer, wide)
            state_in(layer).wait()
            exchange_wait(layer, a2a_s.at[layer], a2a_r.at[layer])
            ring_start(layer)
        with scope("recur"):
            rows[me[0], me[1]] = recur(layer)
        with scope("plane"):
            plane_start(layer, rows)
        with scope("update"):
            update_state(layer)
        with scope("ring"):
            ring_pass(layer)
            exchange_drain(layer, a2a_s.at[layer], a2a_r.at[layer])
            ring_near(layer)
        with scope("far"):
            ring_far(layer)
        with scope("plane_wait"):
            plane_wait(layer, rows)
        with scope("ring_done"):
            ring_done(layer)
        with scope("output"):
            result = output(layer, rows)
            if layer == 0:
                g2[me[0], me[1], me[2]] = result
            else:
                mixed_out[...] = result
        with scope("drain"):
            if layer == 0:
                stage_one(1, g2)
            plane_drain(layer, rows)
            ring_drain(layer)


def flush(mixed, updated, mixed_out, state_out, sems):
    copies = [
        pltpu.make_async_copy(
            updated.at[layer, pl.ds(8 * part, 8)], state_out.at[layer, pl.ds(8 * part, 8)], sems.at[layer, part]
        )
        for layer in range(2)
        for part in range(4)
    ]
    for copy in copies:
        copy.start()
    mixed_out[...] = mixed[...]
    for copy in copies:
        copy.wait()


def local(tokens, lengths, norm_gain, *rest):
    weights = [jnp.swapaxes(weight, 1, 2) for weight in rest[:7]]
    decay_base, rate_base, group_gain, state = rest[7:]
    operands = [tokens, lengths.reshape(1, 32), norm_gain, *weights, decay_base, rate_base, group_gain, state]
    operands = [pltpu.with_memory_space_constraint(operand, pltpu.HBM) for operand in operands]
    vmem = pl.BlockSpec(memory_space=pltpu.VMEM)
    anywhere = pl.BlockSpec(memory_space=pltpu.HBM)
    dma = pltpu.SemaphoreType.DMA
    mixed, updated = pl.pallas_call(
        kernel,
        out_shape=(
            jax.ShapeDtypeStruct((32, 256), BF16),
            jax.ShapeDtypeStruct(state.shape, F32),
        ),
        in_specs=[anywhere] * 14,
        out_specs=(vmem, vmem),
        scratch_shapes=[
            pltpu.VMEM((4, 4, 4, 32, 256), BF16),
            pltpu.VMEM((4, 4, 32, 256), BF16),
            pltpu.VMEM((4, 4, 4, 32, 256), BF16),
            pltpu.VMEM((4, 4, 32, 256), BF16),
            pltpu.VMEM((2, 12, 32, 4096), BF16),
            pltpu.VMEM((2, 4, 2, 32, 4096), BF16),
            pltpu.VMEM((2, 4, 32, 384), BF16),
            pltpu.VMEM((2, 4, 32, 384), BF16),
            pltpu.VMEM((4, 64, 32), F32),
            pltpu.VMEM((4, 32, 64), F32),
            pltpu.VMEM((4, 32, 64), F32),
            pltpu.VMEM((1, 32), jnp.int32),
            pltpu.VMEM((2, 4096), F32),
            pltpu.VMEM((2, 256), F32),
            pltpu.VMEM((2, 256), F32),
            pltpu.VMEM((2, 256), F32),
            dma,
            dma((5,)),
            dma((2, 7)),
            dma((2, 7)),
            dma((2, 7)),
            dma((2,)),
            dma((2, 4, 3)),
            dma((2, 4, 12)),
            dma((2, 2)),
            dma((2, 15)),
            dma((2, 6)),
            dma((2, 6)),
            dma((2, 3)),
            dma((2, 3)),
            dma((2, 3)),
            dma((2, 3)),
        ],
        compiler_params=pltpu.CompilerParams(
            collective_id=0, has_side_effects=True, vmem_limit_bytes=24 * 1024 * 1024
        ),
    )(*operands)
    updated = pltpu.with_memory_space_constraint(updated, pltpu.VMEM)
    return pl.pallas_call(
        flush,
        out_shape=(
            jax.ShapeDtypeStruct((32, 256), BF16),
            jax.ShapeDtypeStruct(state.shape, F32),
        ),
        in_specs=[vmem, vmem],
        out_specs=(vmem, anywhere),
        scratch_shapes=[dma((2, 4))],
        compiler_params=pltpu.CompilerParams(vmem_limit_bytes=1024 * 1024),
    )(mixed, updated)


def solution(mesh):
    finer = Mesh(mesh.devices.reshape(4, 4, 4, 2), ("z", "y", "x", "core"))
    tp, dp = ("z", "y"), ("x", "core")
    weight = P(None, None, tp + dp)
    vector = P(None, tp)
    states = P(None, dp, tp, None, None)
    in_specs = (P(dp, tp), P(dp), P()) + (weight,) * 7 + (vector,) * 3 + (states,)
    return jax.shard_map(
        local, mesh=finer, in_specs=in_specs, out_specs=(P(dp, tp), states), check_vma=False
    )
```

```python
import math

import jax
import jax.numpy as jnp
from jax import lax
from jax.experimental import pallas as pl
from jax.experimental.pallas import tpu as pltpu
from jax.sharding import Mesh
from jax.sharding import PartitionSpec as P

STEP = 16
RMS_EPS = 1e-06
GROUP_EPS = 0.00064
MESH = pl.DeviceIdType.MESH
AXES = ("z", "y", "x")
PARTS = (
    ((0, 24), (0, 128), (1, 2), 0),
    ((0, 24), (128, 128), (0, 2), 1),
    ((24, 8), (0, 256), (0, 1), 2),
)
PLANE = sorted(
    [(dz, dy) for dz in range(4) for dy in range(4) if dz or dy],
    key=lambda offset: -min(offset[0], 4 - offset[0]) - min(offset[1], 4 - offset[1]),
)
NT = (((1,), (1,)), ((), ()))
F32 = jnp.float32
BF16 = jnp.bfloat16
DECAY_SCALE = math.exp(-0.5)


def kernel(
    tokens,
    lengths_hbm,
    norm_gain_hbm,
    w_recept,
    w_key,
    w_value,
    w_decay,
    w_rate,
    w_gate,
    w_out,
    decay_base_hbm,
    rate_base_hbm,
    group_gain_hbm,
    state,
    mixed_out,
    st,
    g0,
    g1,
    g2,
    g3,
    wp,
    wo,
    a2a_s,
    a2a_r,
    u_ref,
    w_ref,
    kl_ref,
    lengths,
    norm_gain,
    decay_base,
    rate_base,
    group_gain,
    tok_sem,
    small_sem,
    loc_sem,
    sib_send,
    sib_recv,
    st_sem,
    g_send,
    g_recv,
    p_send,
    p_recv,
    r_send,
    r_recv,
    d_send,
    d_recv,
    x_send,
    x_recv,
):
    me = tuple(lax.axis_index(axis) for axis in AXES)
    core = lax.axis_index("core")
    weights = (w_recept, w_key, w_value, w_decay, w_rate, w_gate, w_out)

    def peer(dim, step):
        return lax.rem(me[dim] + step, 4)

    def device(dim, step):
        return {AXES[dim]: peer(dim, step)}

    def plane_device(dims, one, two):
        return {AXES[dims[0]]: peer(dims[0], one), AXES[dims[1]]: peer(dims[1], two)}

    sibling = {"core": 1 - core}

    def remote(src, dst, send, recv, where):
        return pltpu.make_async_remote_copy(
            src_ref=src, dst_ref=dst, send_sem=send, recv_sem=recv, device_id=where, device_id_type=MESH
        )

    own = pltpu.make_async_copy(tokens, g0.at[me[0], me[1], me[2]], tok_sem)
    own.start()

    def weight_dst(layer, mat):
        if mat == 6:
            return wo.at[layer, me[2], core]
        return wp.at[layer, 2 * mat + core]

    def weight_src(layer, mat):
        return weights[mat].at[layer]

    def local_weight(layer, mat):
        return pltpu.make_async_copy(
            weight_src(layer, mat), weight_dst(layer, mat), loc_sem.at[layer, mat]
        )

    def sibling_weight(layer, mat):
        return remote(
            weight_src(layer, mat),
            weight_dst(layer, mat),
            sib_send.at[layer, mat],
            sib_recv.at[layer, mat],
            sibling,
        )

    def state_in(layer):
        return pltpu.make_async_copy(state.at[layer], st.at[layer], st_sem.at[layer])

    barrier = pltpu.get_barrier_semaphore()
    partners = [device(dim, step) for dim in range(3) for step in range(1, 4)] + [sibling]
    for dims in ((0, 1), (0, 2), (1, 2)):
        partners += [plane_device(dims, *offset) for offset in PLANE if min(offset) > 0]
    for partner in partners:
        pl.semaphore_signal(barrier, inc=1, device_id=partner, device_id_type=MESH)
    for mat in range(6):
        local_weight(0, mat).start()
    small = [
        pltpu.make_async_copy(src, dst, small_sem.at[idx])
        for idx, (src, dst) in enumerate(
            (
                (norm_gain_hbm, norm_gain),
                (lengths_hbm, lengths),
                (decay_base_hbm, decay_base),
                (rate_base_hbm, rate_base),
                (group_gain_hbm, group_gain),
            )
        )
    ]
    for copy in small:
        copy.start()
    with jax.named_scope("barrier"):
        pl.semaphore_wait(barrier, len(partners))

    def region(buf, part, sel):
        rows, cols, _, _ = PARTS[part]
        return buf.at[tuple(pl.ds(*sel[dim]) for dim in range(3)) + (pl.ds(*rows), pl.ds(*cols))]

    def chosen(parts):
        return [parts.get(dim, (me[dim], 1)) for dim in range(3)]

    def send(gid, buf, part, stage, slot, sel, where):
        block = region(buf, part, chosen(sel))
        remote(block, block, g_send.at[gid, part, stage], g_recv.at[gid, part, slot], where).start()

    def arrived(gid, buf, part, slot, sel):
        block = region(buf, part, chosen(sel))
        remote(block, block, g_send.at[gid, part, 0], g_recv.at[gid, part, slot], sibling).wait_recv()

    def wide_one(gid, buf):
        for one, two in PLANE:
            for part, (_, _, dims, _) in enumerate(PARTS):
                send(gid, buf, part, min(one, 1), 4 * one + two - 1, {}, plane_device(dims, one, two))

    def halves(part, step):
        _, _, dims, ring = PARTS[part]
        place = {dims[1]: (0, 4)}
        if step:
            place[ring] = (peer(ring, step), 1)
        return {**place, dims[0]: (0, 2)}, {**place, dims[0]: (2, 2)}

    def wide_two(gid, buf):
        for part, (_, _, dims, ring) in enumerate(PARTS):
            for one, two in PLANE[::-1]:
                place = {dims[0]: (peer(dims[0], 4 - one), 1), dims[1]: (peer(dims[1], 4 - two), 1)}
                arrived(gid, buf, part, 4 * one + two - 1, place)
            low, high = halves(part, 0)
            send(gid, buf, part, 2, 15, low, device(ring, 1))
            send(gid, buf, part, 2, 17, high, device(ring, 3))
            send(gid, buf, part, 2, 16, high, device(ring, 1))
            send(gid, buf, part, 2, 18, low, device(ring, 3))

    def wide_three(gid, buf):
        for part, (_, _, dims, ring) in enumerate(PARTS):
            low, _ = halves(part, 3)
            arrived(gid, buf, part, 15, low)
            send(gid, buf, part, 2, 19, low, device(ring, 1))
            _, high = halves(part, 1)
            arrived(gid, buf, part, 17, high)
            send(gid, buf, part, 2, 20, high, device(ring, 3))

    def wide_four(gid, buf):
        for part in range(3):
            arrived(gid, buf, part, 16, halves(part, 3)[1])
            arrived(gid, buf, part, 18, halves(part, 1)[0])
        for part in range(3):
            arrived(gid, buf, part, 19, halves(part, 2)[0])
            arrived(gid, buf, part, 20, halves(part, 2)[1])

    def wide_drain(gid, buf):
        for part, (_, _, dims, ring) in enumerate(PARTS):
            for stage, (one, two, three) in enumerate(((1, 3, 1), (3, 4, 1), (4, 4, 3))):
                sel = {dims[0]: (0, one), dims[1]: (0, two), ring: (0, three)}
                block = region(buf, part, chosen(sel))
                remote(block, block, g_send.at[gid, part, stage], g_recv.at[gid, part, 0], sibling).wait_send()

    def plane_start(pid, buf):
        block = buf.at[me[0], me[1]]
        for dz, dy in PLANE:
            remote(
                block, block, p_send.at[pid, min(dz, 1)], p_recv.at[pid, 4 * dz + dy - 1], plane_device((0, 1), dz, dy)
            ).start()

    def plane_wait(pid, buf):
        for dz, dy in PLANE[::-1]:
            block = buf.at[peer(0, 4 - dz), peer(1, 4 - dy)]
            remote(block, block, p_send.at[pid, 0], p_recv.at[pid, 4 * dz + dy - 1], sibling).wait_recv()

    def plane_drain(pid, buf):
        for idx, block in enumerate((buf.at[pl.ds(0, 1), pl.ds(0, 3)], buf.at[pl.ds(0, 3)])):
            remote(block, block, p_send.at[pid, idx], p_recv.at[pid, 0], sibling).wait_send()

    def half(ref, part):
        return ref.at[pl.ds(16 * part, 16)]

    def ring_start(layer):
        for step, part, slot in ((1, 0, 0), (3, 1, 2), (1, 1, 1), (3, 0, 3)):
            remote(
                half(w_out.at[layer], part),
                half(wo.at[layer, me[2], core], part),
                r_send.at[layer, slot],
                r_recv.at[layer, slot],
                device(2, step),
            ).start()

    RING = ((3, 0), (3, 1), (1, 1), (1, 0), (2, 0), (2, 1))

    def ring_wait(layer, slot):
        step, part = RING[slot]
        piece = half(wo.at[layer, peer(2, step), core], part)
        remote(piece, piece, r_send.at[layer, slot], r_recv.at[layer, slot], sibling).wait_recv()

    def ring_pass(layer):
        for slot, onward, step in ((0, 4, 1), (2, 5, 3)):
            ring_wait(layer, slot)
            source, part = RING[slot]
            piece = half(wo.at[layer, peer(2, source), core], part)
            remote(piece, piece, r_send.at[layer, onward], r_recv.at[layer, onward], device(2, step)).start()

    def across(layer, step, which):
        piece = wo.at[layer, peer(2, step), which]
        return remote(piece, piece, d_send.at[layer, step - 1], d_recv.at[layer, step - 1], sibling)

    def ring_near(layer):
        ring_wait(layer, 1)
        across(layer, 3, core).start()
        ring_wait(layer, 3)
        across(layer, 1, core).start()

    def ring_far(layer):
        ring_wait(layer, 4)
        ring_wait(layer, 5)
        across(layer, 2, core).start()

    def ring_done(layer):
        for step in (3, 1, 2):
            across(layer, step, 1 - core).wait_recv()

    def ring_drain(layer):
        for step in (3, 1, 2):
            across(layer, step, core).wait_send()
        for slot in range(6):
            piece = half(wo.at[layer, 0, 0], 0)
            remote(piece, piece, r_send.at[layer, slot], r_recv.at[layer, slot], sibling).wait_send()

    def exchange(eid, src, dst):
        for step in (1, 3, 2):
            remote(
                src.at[peer(2, step)],
                dst.at[me[2]],
                x_send.at[eid, step - 1],
                x_recv.at[eid, step - 1],
                device(2, step),
            ).start()

    def exchange_wait(eid, src, dst):
        for step in range(1, 4):
            slot = dst.at[peer(2, 4 - step)]
            remote(slot, slot, x_send.at[eid, step - 1], x_recv.at[eid, step - 1], sibling).wait_recv()

    def exchange_drain(eid, src, dst):
        for step in range(1, 4):
            slot = src.at[peer(2, step)]
            remote(slot, slot, x_send.at[eid, step - 1], x_recv.at[eid, step - 1], sibling).wait_send()

    def weights_ready(layer, mats):
        for mat in mats:
            local_weight(layer, mat).wait()
            remote(
                weight_src(layer, mat),
                other_dst(layer, mat),
                sib_send.at[layer, mat],
                sib_recv.at[layer, mat],
                sibling,
            ).wait_recv()

    def other_dst(layer, mat):
        if mat == 6:
            return wo.at[layer, me[2], 1 - core]
        return wp.at[layer, 2 * mat + 1 - core]

    def scale_weights(layer):
        def body(idx, carry):
            for part in range(4):
                cols = slice(1024 * part, 1024 * (part + 1))
                gain = norm_gain[layer : layer + 1, cols]
                wp[layer, idx, :, cols] = (wp[layer, idx, :, cols].astype(F32) * gain).astype(BF16)
            return carry

        lax.fori_loop(0, 12, body, 0)

    ones = jnp.ones((8, 256), BF16)

    def project(layer, buf):
        acc = jnp.zeros((384, 128), F32)
        squares = jnp.zeros((8, 128), F32)
        for group in range(16):
            weight = wp[layer, :, :, 256 * group : 256 * (group + 1)].reshape(384, 256)
            block = buf[group // 4, group % 4].reshape(128, 256)
            acc += lax.dot_general(weight, block, NT, preferred_element_type=F32)
            squares += lax.dot_general(ones, block * block, NT, preferred_element_type=F32)
        factor = lax.rsqrt(squares[0:1, :] * (1.0 / 4096) + RMS_EPS)
        rows = jnp.transpose(acc * factor).astype(BF16)
        a2a_s[layer] = rows.reshape(4, 32, 384)

    def head_parts(row):
        return [row[:, 64 * head : 64 * (head + 1)] for head in range(4)]

    row_of = lax.broadcasted_iota(jnp.int32, (8, 64), 0)

    def recur(layer):
        lane_len = lengths[...].astype(F32)
        diag = lax.broadcasted_iota(jnp.int32, (32, 32), 0) == lax.broadcasted_iota(jnp.int32, (32, 32), 1)
        active = jnp.sum(jnp.where(diag, lane_len, 0.0), axis=1, keepdims=True) > STEP
        decay_parts = head_parts(decay_base[layer : layer + 1, :])
        rate_parts = head_parts(rate_base[layer : layer + 1, :])
        gain_parts = head_parts(group_gain[layer : layer + 1, :])
        results = []
        for head in range(4):
            tile = a2a_r[layer, head].astype(F32)
            recept, key, value, decay, rate, gate = [
                tile[:, 64 * mat : 64 * (mat + 1)] for mat in range(6)
            ]
            size = jnp.maximum(jnp.sqrt(jnp.sum(key * key, axis=1, keepdims=True)), 1e-12)
            unit = key / size
            keep = jnp.exp(-DECAY_SCALE * jax.nn.sigmoid(decay_parts[head] + decay))
            unit_rate = unit * jax.nn.sigmoid(rate_parts[head] + rate)
            beta = jnp.sum(unit_rate * recept, axis=1, keepdims=True)
            probe = (keep * recept).astype(BF16)
            unit_b = unit.astype(BF16)
            along, read = [], []
            for octet in range(4):
                rows = slice(8 * octet, 8 * octet + 8)
                left = jnp.concatenate([unit_b[rows], probe[rows]], axis=0)
                sum_a = jnp.zeros((8, 64), F32)
                sum_r = jnp.zeros((8, 64), F32)
                for low in range(8):
                    seq = 8 * octet + low
                    matrix = st[layer, seq, head].astype(BF16)
                    both = lax.dot_general(left, matrix, NT, preferred_element_type=F32)
                    sum_a = jnp.where(row_of == low, both[0:8], sum_a)
                    sum_r = jnp.where(row_of == low, both[8:16], sum_r)
                along.append(sum_a)
                read.append(sum_r)
            delta = size * value - jnp.concatenate(along, axis=0)
            readout = jnp.concatenate(read, axis=0) + delta * beta
            centre = jnp.mean(readout, axis=1, keepdims=True)
            moved = readout - centre
            spread = jnp.mean(moved * moved, axis=1, keepdims=True)
            normal = moved * lax.rsqrt(spread + GROUP_EPS) * gain_parts[head]
            results.append(jnp.where(active, normal * jax.nn.sigmoid(gate), 0.0))
            u_ref[head] = jnp.transpose(delta)
            w_ref[head] = jnp.where(active, keep, 1.0)
            kl_ref[head] = jnp.where(active, unit_rate, 0.0)
        return jnp.concatenate(results, axis=1).astype(BF16)

    def update_state(layer):
        for head in range(4):
            column = u_ref[head]
            for seq in range(32):
                st[layer, seq, head] = (
                    st[layer, seq, head] * w_ref[head, seq : seq + 1, :]
                    + column[:, seq : seq + 1] * kl_ref[head, seq : seq + 1, :]
                )

    def output(layer, buf):
        acc = jnp.zeros((256, 32), F32)
        for group in range(16):
            weight = wo[layer, :, :, :, 256 * group : 256 * (group + 1)].reshape(256, 256)
            acc += lax.dot_general(weight, buf[group // 4, group % 4], NT, preferred_element_type=F32)
        return jnp.transpose(acc).astype(BF16)

    def start_weights(layer, mats):
        for mat in mats:
            local_weight(layer, mat).start()
            sibling_weight(layer, mat).start()

    def drain_weights(layer):
        for mat in range(7):
            sibling_weight(layer, mat).wait_send()

    scope = jax.named_scope
    with scope("own"):
        own.wait()
    with scope("g0_one"):
        wide_one(0, g0)
        for mat in range(6):
            sibling_weight(0, mat).start()
        ring_start(0)
        state_in(0).start()
        start_weights(0, (6,))
    buffers = ((g0, g1), (g2, g3))
    for layer in range(2):
        wide, rows = buffers[layer]
        with scope("two"):
            if layer == 0:
                for copy in small:
                    copy.wait()
            wide_two(layer, wide)
            if layer == 0:
                start_weights(1, range(7))
                state_in(1).start()
        with scope("scale"):
            weights_ready(layer, range(7))
            scale_weights(layer)
            drain_weights(layer)
        with scope("three"):
            wide_three(layer, wide)
        with scope("four"):
            wide_four(layer, wide)
        with scope("project"):
            project(layer, wide)
        with scope("exchange"):
            exchange(layer, a2a_s.at[layer], a2a_r.at[layer])
            a2a_r[layer, me[2]] = a2a_s[layer, me[2]]
            wide_drain(layer, wide)
            state_in(layer).wait()
            exchange_wait(layer, a2a_s.at[layer], a2a_r.at[layer])
        with scope("ring"):
            ring_pass(layer)
            ring_near(layer)
        with scope("recur"):
            rows[me[0], me[1]] = recur(layer)
        with scope("plane"):
            plane_start(layer, rows)
            if layer == 0:
                ring_start(1)
        with scope("update"):
            update_state(layer)
        with scope("far"):
            ring_far(layer)
            exchange_drain(layer, a2a_s.at[layer], a2a_r.at[layer])
        with scope("plane_wait"):
            plane_wait(layer, rows)
        with scope("ring_done"):
            ring_done(layer)
        with scope("output"):
            result = output(layer, rows)
            if layer == 0:
                g2[me[0], me[1], me[2]] = result
            else:
                mixed_out[...] = result
        with scope("drain"):
            if layer == 0:
                wide_one(1, g2)
            plane_drain(layer, rows)
            ring_drain(layer)


def flush(mixed, updated, mixed_out, state_out, sems):
    copies = [
        pltpu.make_async_copy(
            updated.at[layer, pl.ds(8 * part, 8)], state_out.at[layer, pl.ds(8 * part, 8)], sems.at[layer, part]
        )
        for layer in range(2)
        for part in range(4)
    ]
    for copy in copies:
        copy.start()
    mixed_out[...] = mixed[...]
    for copy in copies:
        copy.wait()


def local(tokens, lengths, norm_gain, *rest):
    weights = [jnp.swapaxes(weight, 1, 2) for weight in rest[:7]]
    decay_base, rate_base, group_gain, state = rest[7:]
    operands = [tokens, lengths.reshape(1, 32), norm_gain, *weights, decay_base, rate_base, group_gain, state]
    operands = [pltpu.with_memory_space_constraint(operand, pltpu.HBM) for operand in operands]
    vmem = pl.BlockSpec(memory_space=pltpu.VMEM)
    anywhere = pl.BlockSpec(memory_space=pltpu.HBM)
    dma = pltpu.SemaphoreType.DMA
    mixed, updated = pl.pallas_call(
        kernel,
        out_shape=(
            jax.ShapeDtypeStruct((32, 256), BF16),
            jax.ShapeDtypeStruct(state.shape, F32),
        ),
        in_specs=[anywhere] * 14,
        out_specs=(vmem, vmem),
        scratch_shapes=[
            pltpu.VMEM((4, 4, 4, 32, 256), BF16),
            pltpu.VMEM((4, 4, 32, 256), BF16),
            pltpu.VMEM((4, 4, 4, 32, 256), BF16),
            pltpu.VMEM((4, 4, 32, 256), BF16),
            pltpu.VMEM((2, 12, 32, 4096), BF16),
            pltpu.VMEM((2, 4, 2, 32, 4096), BF16),
            pltpu.VMEM((2, 4, 32, 384), BF16),
            pltpu.VMEM((2, 4, 32, 384), BF16),
            pltpu.VMEM((4, 64, 32), F32),
            pltpu.VMEM((4, 32, 64), F32),
            pltpu.VMEM((4, 32, 64), F32),
            pltpu.VMEM((1, 32), jnp.int32),
            pltpu.VMEM((2, 4096), F32),
            pltpu.VMEM((2, 256), F32),
            pltpu.VMEM((2, 256), F32),
            pltpu.VMEM((2, 256), F32),
            dma,
            dma((5,)),
            dma((2, 7)),
            dma((2, 7)),
            dma((2, 7)),
            dma((2,)),
            dma((2, 3, 3)),
            dma((2, 3, 21)),
            dma((2, 2)),
            dma((2, 15)),
            dma((2, 6)),
            dma((2, 6)),
            dma((2, 3)),
            dma((2, 3)),
            dma((2, 3)),
            dma((2, 3)),
        ],
        compiler_params=pltpu.CompilerParams(
            collective_id=0, has_side_effects=True, vmem_limit_bytes=24 * 1024 * 1024
        ),
    )(*operands)
    updated = pltpu.with_memory_space_constraint(updated, pltpu.VMEM)
    return pl.pallas_call(
        flush,
        out_shape=(
            jax.ShapeDtypeStruct((32, 256), BF16),
            jax.ShapeDtypeStruct(state.shape, F32),
        ),
        in_specs=[vmem, vmem],
        out_specs=(vmem, anywhere),
        scratch_shapes=[dma((2, 4))],
        compiler_params=pltpu.CompilerParams(vmem_limit_bytes=1024 * 1024),
    )(mixed, updated)


def solution(mesh):
    finer = Mesh(mesh.devices.reshape(4, 4, 4, 2), ("z", "y", "x", "core"))
    tp, dp = ("z", "y"), ("x", "core")
    weight = P(None, None, tp + dp)
    vector = P(None, tp)
    states = P(None, dp, tp, None, None)
    in_specs = (P(dp, tp), P(dp), P()) + (weight,) * 7 + (vector,) * 3 + (states,)
    return jax.shard_map(
        local, mesh=finer, in_specs=in_specs, out_specs=(P(dp, tp), states), check_vma=False
    )
```
